32 devices in a mesh: dp: 4 (over y, x), kv: 4 (over z), tp: 2 (over core).
Axes of the slice: x: 2, y: 2, z: 4, core: 2. Of those that a mesh axis runs over, the one named last changes fastest.
Arguments:
- tokens: bfloat16 [32, 2048], P('dp', ('kv', 'tp')), as said below
- first_gain: float32 [2048], replicated, may hold values from 0.1 to 1.9
- first_gate: bfloat16 [2048, 5632], P(None, ('kv', 'tp')), may hold values from -0.125 to 0.125
- first_up: bfloat16 [2048, 5632], P(None, ('kv', 'tp')), may hold values from -0.125 to 0.125
- first_down: bfloat16 [5632, 2048], P(('kv', 'tp')), may hold values from -0.109375 to 0.109375
- mix_gain: float32 [2048], P(('kv', 'tp')), may hold values from 0.1 to 1.9
- w_input: bfloat16 [2048, 2048], P(('kv', 'tp')), may hold values from -0.125 to 0.125
- w_outgate: bfloat16 [2048, 2048], P(('kv', 'tp')), may hold values from -0.125 to 0.125
- w_write: bfloat16 [2048, 512], P(('kv', 'tp')), may hold values from -0.125 to 0.125
- w_read: bfloat16 [2048, 512], P(('kv', 'tp')), may hold values from -0.125 to 0.125
- w_step: bfloat16 [2048, 32], P(('kv', 'tp')), may hold values from -0.125 to 0.125
- conv_taps: bfloat16 [4, 3072], replicated, may hold values from -3 to 3
- conv_history: bfloat16 [32, 3, 3072], P(('dp', 'kv', 'tp')), may hold values from -6 to 6
- step_bias: float32 [32], replicated, may hold values from -6 to -1
- rate_log: float32 [32], replicated, may hold values from 0 to 2.77
- mixer_state: float32 [32, 32, 64, 128], P(('dp', 'kv', 'tp')), may hold values from -4 to 4
- group_gain: float32 [2048], replicated, may hold values from 0.1 to 1.9
- w_output: bfloat16 [2048, 2048], P(None, ('kv', 'tp')), may hold values from -0.125 to 0.125
- second_gain: float32 [2048], replicated, may hold values from 0.1 to 1.9
- second_gate: bfloat16 [2048, 5632], P(None, ('kv', 'tp')), may hold values from -0.125 to 0.125
- second_up: bfloat16 [2048, 5632], P(None, ('kv', 'tp')), may hold values from -0.125 to 0.125
- second_down: bfloat16 [5632, 2048], P(('kv', 'tp')), may hold values from -0.109375 to 0.109375
Outputs:
- layer_out: bfloat16 [32, 2048], P('dp', ('kv', 'tp'))
- state_out: float32 [32, 32, 64, 128], P(('dp', 'kv', 'tp'))
- history_out: bfloat16 [32, 3, 3072], P(('dp', 'kv', 'tp'))
The draws below stay inside these ranges and needn't reach their ends.
Inputs may be any that keep to these rules, and one draw needn't show every extreme that they name: `tokens`: channel scales rise along the width.
All inputs are finite; a program needn't handle non-finite values.
Results may differ from the reference program's by a relative error of at most 0.014.
Values may be sent and summed in bfloat16 or wider, within the bound.
A program may use at most 64 MiB of HBM per device.

```python
import math
import jax
import jax.numpy as jnp
from jax import lax

D = 2048
FF = 5632
HEADS = 32
HEAD_DIM = 64
D_STATE = 128
GROUPS = 4
TAPS = 4
BATCH = 32
SSD_WIDTH = 2048
CONV_DIM = 3072


def draw_tokens(key, part):
    column = jnp.exp(jnp.linspace(0.0, math.log(6.0), D)).astype(jnp.float32)
    values = jax.random.normal(key, (BATCH, D), jnp.float32) * column / 3.0
    return values.astype(jnp.bfloat16)


def raised(array, stream_key, source, target, shards_of, factor):
    def block_of(position):
        return (jnp.arange(array.shape[position]) // (array.shape[position] // shards_of)).reshape((-1,) + (1,) * (array.ndim - 1 - position))

    first = jax.random.permutation(stream_key, shards_of)[block_of(target)]
    second = (block_of(target) + shards_of // 2) % shards_of
    return jnp.where((block_of(source) == first) | (block_of(source) == second), factor * array, array)


def levels(own_key, shape, shards, low, top_value):
    def one(axis_at, shards_of):
        steps = jax.random.uniform(jax.random.fold_in(jax.random.fold_in(own_key, 6), axis_at), (shards_of,), jnp.float32, low / len(shards), top_value / len(shards))
        return jnp.repeat(jnp.exp(steps), shape[axis_at] // shards_of).reshape((-1,) + (1,) * (len(shape) - axis_at - 1))

    factor_of = one(*shards[0])
    for cut in shards[1:]:
        factor_of = factor_of * one(*cut)
    return factor_of


def bell_draw(key, dims, scale, most, pieces=(), kind=jnp.bfloat16):
    result = jax.random.normal(key, dims, jnp.float32) * scale
    if len(pieces) > 0:
        result = levels(key, dims, pieces, -0.22, 0.18) * result
    return jnp.clip(result, min=-most, max=most).astype(kind)


def noise_with(stream_key, dims, spread, reach, cuts, heavy, dtype=jnp.bfloat16):
    drawn = spread * jax.random.normal(stream_key, dims, jnp.float32)
    if cuts:
        drawn = drawn * levels(stream_key, dims, cuts, -0.22, 0.18)
    return jnp.clip(raised(drawn, jax.random.fold_in(stream_key, 3), *heavy), -reach, reach).astype(dtype)


def setup_inputs(seed: int = 0) -> dict:
    splits = jax.random.split(jax.random.key(seed), 23)
    tokens = draw_tokens(jax.random.fold_in(splits[22], 71), 0)
    first_gain = jnp.clip(1.0 + 0.18 * jax.random.normal(splits[1], (D,), jnp.float32), 0.1, 1.9)
    first_gate = bell_draw(splits[2], (D, FF), D ** -0.5, 0.125, ((1, 8),))
    first_up = bell_draw(splits[3], (D, FF), D ** -0.5, 0.125, ((1, 8),))
    first_down = noise_with(splits[4], (FF, D), FF ** -0.5, 0.109375, ((0, 8),), (0, 1, 8, 2.0))
    mix_gain = jnp.clip(1.0 + 0.18 * jax.random.normal(splits[5], (D,), jnp.float32), 0.1, 1.9)
    w_input = bell_draw(splits[6], (D, SSD_WIDTH), D ** -0.5, 0.125, ((0, 8),))
    w_outgate = bell_draw(splits[7], (D, SSD_WIDTH), D ** -0.5, 0.125, ((0, 8),))
    w_write = bell_draw(splits[8], (D, GROUPS * D_STATE), D ** -0.5, 0.125, ((0, 8),))
    w_read = bell_draw(splits[9], (D, GROUPS * D_STATE), D ** -0.5, 0.125, ((0, 8),))
    w_step = bell_draw(splits[10], (D, HEADS), D ** -0.5, 0.125, ((0, 8),))
    conv_taps = bell_draw(splits[11], (TAPS, CONV_DIM), 0.5, 3.0)
    conv_history = bell_draw(splits[12], (BATCH, TAPS - 1, CONV_DIM), 1.0, 6.0, ((0, 32),))
    step_bias = jnp.clip(jax.random.uniform(splits[13], (HEADS,), jnp.float32, -6.0, -1.0), -6.0, -1.0)
    rate_log = jnp.clip(jax.random.uniform(splits[14], (HEADS,), jnp.float32, 0.0, 2.77), 0.0, 2.77)
    mixer_state = bell_draw(splits[15], (BATCH, HEADS, HEAD_DIM, D_STATE), 0.5, 4.0, ((0, 32),), jnp.float32)
    group_gain = jnp.clip(1.0 + 0.18 * jax.random.normal(splits[16], (SSD_WIDTH,), jnp.float32), 0.1, 1.9)
    w_output = bell_draw(splits[17], (SSD_WIDTH, D), SSD_WIDTH ** -0.5, 0.125, ((1, 8),))
    second_gain = jnp.clip(1.0 + 0.18 * jax.random.normal(splits[18], (D,), jnp.float32), 0.1, 1.9)
    second_gate = bell_draw(splits[19], (D, FF), D ** -0.5, 0.125, ((1, 8),))
    second_up = bell_draw(splits[20], (D, FF), D ** -0.5, 0.125, ((1, 8),))
    second_down = noise_with(splits[21], (FF, D), FF ** -0.5, 0.109375, ((0, 8),), (0, 1, 8, 2.0))
    return dict(tokens=tokens, first_gain=first_gain, first_gate=first_gate, first_up=first_up, first_down=first_down, mix_gain=mix_gain, w_input=w_input, w_outgate=w_outgate, w_write=w_write, w_read=w_read, w_step=w_step, conv_taps=conv_taps, conv_history=conv_history, step_bias=step_bias, rate_log=rate_log, mixer_state=mixer_state, group_gain=group_gain, w_output=w_output, second_gain=second_gain, second_gate=second_gate, second_up=second_up, second_down=second_down)


EPS = 1e-06

def half_block(resid, gain, w_gate, w_up, w_down):
    resid_f = resid.astype(jnp.float32)
    scale = lax.rsqrt(lax.optimization_barrier(jnp.mean(resid_f * resid_f, axis=-1, keepdims=True)) + EPS)
    normed = (resid_f * scale * gain).astype(jnp.bfloat16)
    gate = jnp.dot(normed, w_gate, preferred_element_type=jnp.float32)
    upper = jnp.dot(normed, w_up, preferred_element_type=jnp.float32)
    hidden = (jax.nn.silu(gate) * upper).astype(jnp.bfloat16)
    down = jnp.dot(hidden, w_down, preferred_element_type=jnp.float32)
    return (resid_f + 0.5 * down).astype(jnp.bfloat16)

def reference(tokens, first_gain, first_gate, first_up, first_down, mix_gain, w_input, w_outgate, w_write, w_read, w_step, conv_taps, conv_history, step_bias, rate_log, mixer_state, group_gain, w_output, second_gain, second_gate, second_up, second_down):
    first = half_block(tokens, first_gain, first_gate, first_up, first_down)
    first_f = first.astype(jnp.float32)
    squares = lax.optimization_barrier(jnp.sum(first_f * first_f, axis=1, keepdims=True))
    scale = lax.rsqrt(squares / D + EPS)
    premix = (first_f * mix_gain).astype(jnp.bfloat16)

    def project(weight):
        return (scale * jnp.dot(premix, weight, preferred_element_type=jnp.float32)).astype(jnp.bfloat16)
    inputs = project(w_input)
    outgate = project(w_outgate)
    writes = project(w_write)
    reads = project(w_read)
    steps_raw = project(w_step)
    fresh = jnp.concatenate([inputs, writes, reads], axis=1)
    window = jnp.concatenate([conv_history, fresh[:, None, :]], axis=1)
    history_out = window[:, 1:]
    conv = jax.nn.silu(lax.optimization_barrier(jnp.sum(window.astype(jnp.float32) * conv_taps.astype(jnp.float32)[None], axis=1)))
    count = conv.shape[0]
    per_group = HEADS // GROUPS
    conv_in = conv[:, :SSD_WIDTH].reshape(count, GROUPS, per_group, HEAD_DIM)
    conv_write = conv[:, SSD_WIDTH:SSD_WIDTH + GROUPS * D_STATE].reshape(count, GROUPS, D_STATE)
    conv_read = conv[:, SSD_WIDTH + GROUPS * D_STATE:].reshape(count, GROUPS, D_STATE)
    step = jax.nn.softplus(steps_raw.astype(jnp.float32) + step_bias)
    decay = jnp.exp(-step * jnp.exp(rate_log))
    state = mixer_state.reshape(count, GROUPS, per_group, HEAD_DIM, D_STATE)
    decay_g = decay.reshape(count, GROUPS, per_group)
    step_g = step.reshape(count, GROUPS, per_group)
    written = (step_g[..., None] * conv_in)[..., None] * conv_write[:, :, None, None, :]
    new_state = decay_g[..., None, None] * state + written
    read_out = jnp.einsum('sgjpn,sgn->sgjp', new_state, conv_read, precision=lax.Precision.HIGHEST)
    gated = read_out.reshape(count, SSD_WIDTH) * jax.nn.silu(outgate.astype(jnp.float32))
    blocks = gated.reshape(count, GROUPS, SSD_WIDTH // GROUPS)
    block_scale = lax.rsqrt(lax.optimization_barrier(jnp.mean(blocks * blocks, axis=-1, keepdims=True)) + EPS)
    normed = ((blocks * block_scale).reshape(count, SSD_WIDTH) * group_gain).astype(jnp.bfloat16)
    mixed = jnp.dot(normed, w_output, preferred_element_type=jnp.float32)
    second = (first_f + mixed).astype(jnp.bfloat16)
    layer_out = half_block(second, second_gain, second_gate, second_up, second_down)
    state_out = new_state.reshape(count, HEADS, HEAD_DIM, D_STATE)
    return (layer_out, state_out, history_out)
```

```python
import functools
import math

import jax
import jax.numpy as jnp
from jax import lax
from jax.experimental import pallas as pl
from jax.experimental.pallas import tpu as pltpu
from jax.sharding import PartitionSpec as P

EPS = 1e-06
F32 = jnp.float32
BF16 = jnp.bfloat16
LANES = 128
VMEM_BYTES = 67043328
MESH = pl.DeviceIdType.MESH


def silu(x):
    return x * jax.nn.sigmoid(x)


def dot_rows(left, right):
    contract = (((1,), (1,)), ((), ()))
    return lax.dot_general(left, right, contract, preferred_element_type=F32)


def layer_kernel(
    kv,
    tp,
    heads,
    tokens,
    first_gain,
    first_gate,
    first_up,
    first_down,
    mix_gain,
    w_input,
    w_outgate,
    w_write,
    w_read,
    w_step,
    conv_taps,
    conv_history,
    step_bias,
    rate_log,
    mixer_state,
    group_gain,
    w_output,
    second_gain,
    second_gate,
    second_up,
    second_down,
    layer_out,
    state_out,
    history_out,
    g1,
    wg1,
    wu1,
    wd1,
    mg,
    wi,
    wo,
    ww,
    wr,
    ws,
    taps,
    hist,
    bias,
    rate,
    state,
    ggain,
    wout,
    g2,
    wg2,
    wu2,
    wd2,
    tok_all,
    down_send1,
    down_recv1,
    proj_send,
    proj_recv,
    norm_all,
    sec_all,
    down_send2,
    down_recv2,
    proj_f,
    step_f,
    state_b,
    hist_f,
    taps_f,
    fresh_f,
    dots_f,
    tail_f,
    norm_f,
    load_sem,
    send_sem,
    recv_sem,
):
    n = kv * tp
    rows, chan = tokens.shape
    width = n * chan
    rows_in = w_input.shape[1] // LANES
    rows_map = w_write.shape[1] // LANES
    rows_conv = rows_in + 2 * rows_map
    rows_all = rows_conv + rows_in
    pack = proj_send.shape[1]
    per_row = heads // rows_in
    head_dim = LANES // per_row
    group_rows = rows_in // rows_map

    my_kv = lax.axis_index("kv")
    my_tp = lax.axis_index("tp")
    me = my_kv * tp + my_tp

    if kv == 4:
        half = my_kv // 2
        chips = [my_kv + 1 - 2 * lax.rem(my_kv, 2), 2 - half, 3 - 3 * half]
    else:
        chips = [lax.rem(my_kv + d, kv) for d in range(1, kv)]
    peers = []
    for pk, first_t in [(pk, 0) for pk in reversed(chips)] + [(my_kv, 1)]:
        for t in range(first_t, tp):
            pt = lax.rem(my_tp + t, tp)
            peers.append((pk * tp + pt, {"kv": pk, "tp": pt}))

    loads = {}

    def load(name, src, dst):
        copy = pltpu.make_async_copy(src, dst, load_sem.at[len(loads)])
        copy.start()
        loads[name] = copy

    def ready(*names):
        for name in names:
            loads[name].wait()

    sends = []

    def send(phase, index, src, dst):
        peer, where = peers[index]
        copy = pltpu.make_async_remote_copy(
            src_ref=src,
            dst_ref=dst,
            send_sem=send_sem.at[phase, index],
            recv_sem=recv_sem.at[phase, me],
            device_id=where,
            device_id_type=MESH,
        )
        copy.start()
        sends.append(copy)

    def arrive(phase, index, dst):
        peer, where = peers[index]
        pltpu.make_async_remote_copy(
            src_ref=dst,
            dst_ref=dst,
            send_sem=send_sem.at[phase, index],
            recv_sem=recv_sem.at[phase, peer],
            device_id=where,
            device_id_type=MESH,
        ).wait_recv()

    barrier = pltpu.get_barrier_semaphore()
    for _, where in peers:
        pl.semaphore_signal(barrier, inc=1, device_id=where, device_id_type=MESH)
    load("tokens", tokens, tok_all.at[me])
    load("g1", first_gain, g1)
    load("wg1", first_gate, wg1)
    load("wu1", first_up, wu1)
    load("wd1", first_down, wd1)
    load("mg", mix_gain, mg)
    load("hist", conv_history.at[0], hist)
    load("taps", conv_taps, taps)
    load("bias", step_bias, bias)
    load("rate", rate_log, rate)
    load("ggain", group_gain, ggain)
    load("g2", second_gain, g2)
    ready("tokens")
    pl.semaphore_wait(barrier, n - 1)
    for i in range(n - 1):
        send(0, i, tok_all.at[me], tok_all.at[me])
    load("wi", w_input, wi)
    load("ww", w_write, ww)
    load("wr", w_read, wr)
    load("wo", w_outgate, wo)
    load("ws", w_step, ws)
    load("state", mixer_state, state)

    ready("hist", "taps")
    for k in range(rows_conv):
        lanes = slice(k * LANES, (k + 1) * LANES)
        hist_f[:, k, :] = hist[:, lanes].astype(F32)
        taps_f[:, k, :] = taps[:, lanes].astype(F32)

    def half_block(phase, slots, gain, w_gate, w_up, w_down, names, down_send, down_recv, fill):
        ready(*names[:3])
        block = tp * chan
        power = gate = upper = None
        for c, pk in enumerate([my_kv] + chips):
            size = tp - 1 if c == 0 else tp
            start = len(peers) - (tp - 1) - c * tp
            for i in range(start, start + size):
                arrive(phase, i, slots.at[peers[i][0]])
            resid = jnp.concatenate([slots[pk * tp + t] for t in range(tp)], axis=1).astype(F32)
            columns = pl.ds(pl.multiple_of(pk * block, block), block)
            weighted = (resid * gain[:, columns]).astype(BF16)
            terms = (
                resid * resid,
                dot_rows(weighted, w_gate[:, columns]),
                dot_rows(weighted, w_up[:, columns]),
            )
            if c == 0:
                power, gate, upper = terms
            else:
                power, gate, upper = power + terms[0], gate + terms[1], upper + terms[2]
        scale = lax.rsqrt(jnp.sum(power, axis=1, keepdims=True) / width + EPS)
        hidden = (silu(gate * scale) * (upper * scale)).astype(BF16)
        ready(names[3])

        def part(dest):
            columns = pl.ds(pl.multiple_of(dest * chan, chan), chan)
            return jnp.dot(hidden, w_down[:, columns], preferred_element_type=F32)

        for i, (peer, _) in enumerate(peers):
            down_send[i] = part(peer).astype(BF16)
            send(phase + 1, i, down_send.at[i], down_recv.at[me])
        total = part(me)
        fill()
        for i in reversed(range(n - 1)):
            peer = peers[i][0]
            arrive(phase + 1, i, down_recv.at[peer])
            total = total + down_recv[peer].astype(F32)
        own = slots[me].astype(F32)
        return (own + 0.5 * total).astype(BF16)

    load("wout", w_output, wout)
    load("wg2", second_gate, wg2)
    load("wu2", second_up, wu2)
    load("wd2", second_down, wd2)

    def round_state():
        ready("state")
        state_b[...] = state[...].astype(BF16)

    first = half_block(
        0,
        tok_all,
        g1,
        wg1,
        wu1,
        wd1,
        ("g1", "wg1", "wu1", "wd1"),
        down_send1,
        down_recv1,
        round_state,
    )
    first_f = first.astype(F32)

    ready("mg", "wi", "ww", "wr", "wo", "ws")
    squares = jnp.sum(first_f * first_f, axis=1, keepdims=True)
    premix = (first_f * mg[...]).astype(BF16)
    row = 0
    for weight in (wi, ww, wr, wo):
        part = jnp.dot(premix, weight[...], preferred_element_type=F32)
        for k in range(weight.shape[1] // LANES):
            proj_f[:, row, :] = part[:, k * LANES : (k + 1) * LANES]
            row += 1
    step_f[...] = jnp.zeros_like(step_f)
    step_f[:, :heads] = dot_rows(premix, ws[...])
    high = squares.astype(BF16).astype(F32)
    lane = lax.broadcasted_iota(jnp.int32, (rows, LANES), 1)
    last = jnp.where(lane == heads, high, step_f[...])
    last = jnp.where(lane == heads + 1, squares - high, last)
    proj_f[:, row, :] = last
    for k in range(row + 1, pack):
        proj_f[:, k, :] = jnp.zeros((rows, LANES), F32)
    for i, (peer, _) in enumerate(peers):
        proj_send[i] = proj_f[peer].astype(BF16)
        send(2, i, proj_send.at[i], proj_recv.at[me])
    summed = proj_f[me]
    for i in reversed(range(n - 1)):
        peer = peers[i][0]
        arrive(2, i, proj_recv.at[peer])
        summed = summed + proj_recv[peer].astype(F32)

    tail = summed[rows_all : rows_all + 1]
    own_squares = tail[:, heads : heads + 1] + tail[:, heads + 1 : heads + 2]
    scale = lax.rsqrt(own_squares / width + EPS)
    scaled = (scale * summed).astype(BF16).astype(F32)
    fresh = scaled[:rows_conv]
    conv = taps_f[3] * fresh
    for k in range(3):
        conv = conv + taps_f[k] * hist_f[k]
    conv = silu(conv)
    conv_in = conv[:rows_in]
    conv_write = conv[rows_in : rows_in + rows_map]
    conv_read = conv[rows_in + rows_map :]
    outgate = scaled[rows_conv:rows_all]

    ready("bias", "rate", "ggain")
    steps_raw = scaled[rows_all : rows_all + 1, :heads] + bias[...]
    step_row = jnp.maximum(steps_raw, 0.0) + jnp.log1p(jnp.exp(-jnp.abs(steps_raw)))
    decay_row = jnp.exp(-step_row * jnp.exp(rate[...]))
    r_id = lax.broadcasted_iota(jnp.int32, (rows_in, heads), 0)
    h_id = lax.broadcasted_iota(jnp.int32, (rows_in, heads), 1)
    wide_lane = lax.broadcasted_iota(jnp.int32, (rows_in, LANES), 1)

    def spread(values):
        out = jnp.zeros((rows_in, LANES), F32)
        for k in range(per_row):
            mine = jnp.where(h_id == r_id * per_row + k, values, 0.0)
            column = jnp.sum(mine, axis=1, keepdims=True)
            inside = (wide_lane >= k * head_dim) & (wide_lane < (k + 1) * head_dim)
            out = jnp.where(inside, column, out)
        return out

    step_c = spread(step_row)
    decay_c = spread(decay_row)
    fed = step_c * conv_in

    read_high = conv_read.astype(BF16).astype(F32)
    lhs = jnp.concatenate([read_high, conv_read - read_high], axis=0).astype(BF16)
    dots = dot_rows(lhs, state_b[...])
    pieces = []
    for r in range(rows_in):
        g = r // group_rows
        lanes = slice(r * LANES, (r + 1) * LANES)
        pieces.append(dots[g : g + 1, lanes] + dots[rows_map + g : rows_map + g + 1, lanes])
    old_read = jnp.concatenate(pieces, axis=0)
    both = jnp.sum(conv_write * conv_read, axis=1, keepdims=True)
    both = jnp.concatenate(
        [jnp.broadcast_to(both[g : g + 1], (group_rows, 1)) for g in range(rows_map)], axis=0
    )
    read_out = decay_c * old_read + fed * both
    gated = read_out * silu(outgate)
    power = jnp.sum(gated * gated, axis=1, keepdims=True)
    power = jnp.concatenate(
        [
            jnp.broadcast_to(
                jnp.sum(power[g * group_rows : (g + 1) * group_rows], axis=0, keepdims=True),
                (group_rows, 1),
            )
            for g in range(rows_map)
        ],
        axis=0,
    )
    block_scale = lax.rsqrt(power / (group_rows * LANES) + EPS)
    norm_all[me] = (gated * block_scale * ggain[...]).astype(BF16)
    for i in range(n - 1):
        send(3, i, norm_all.at[me], norm_all.at[me])

    decay_t = jnp.transpose(decay_c)
    fed_t = jnp.transpose(fed)
    for r in range(rows_in):
        g = r // group_rows
        block = slice(r * LANES, (r + 1) * LANES)
        state_out[block] = (
            decay_t[:, r : r + 1] * state[block]
            + fed_t[:, r : r + 1] * conv_write[g : g + 1]
        )
    fresh_f[...] = fresh
    kept = hist.shape[0]
    tail_f[0 : kept - 1, :] = hist[...].astype(F32)[1:]
    for k in range(rows_conv):
        tail_f[kept - 1 : kept, k * LANES : (k + 1) * LANES] = fresh_f[k : k + 1, :]
    history_out[...] = tail_f[...].astype(BF16)

    for i in reversed(range(n - 1)):
        arrive(3, i, norm_all.at[peers[i][0]])
    for j in range(n):
        norm_f[j] = norm_all[j].astype(F32)
    normed = jnp.concatenate([norm_f[:, r, :] for r in range(rows_in)], axis=1).astype(BF16)
    ready("wout")
    mixed = jnp.dot(normed, wout[...], preferred_element_type=F32)
    sec_all[me] = (first_f + mixed).astype(BF16)
    for i in range(n - 1):
        send(4, i, sec_all.at[me], sec_all.at[me])
    layer_out[...] = half_block(
        4,
        sec_all,
        g2,
        wg2,
        wu2,
        wd2,
        ("g2", "wg2", "wu2", "wd2"),
        down_send2,
        down_recv2,
        lambda: None,
    )
    for copy in sends:
        copy.wait_send()


def write_kernel(layer_in, state_in, history_in, layer_out, state_out, history_out, sem):
    copies = [
        pltpu.make_async_copy(state_in, state_out, sem.at[0]),
        pltpu.make_async_copy(layer_in, layer_out, sem.at[1]),
        pltpu.make_async_copy(history_in, history_out.at[0], sem.at[2]),
    ]
    for copy in copies:
        copy.start()
    for copy in copies:
        copy.wait()


NAMES = (
    "tokens",
    "first_gain",
    "first_gate",
    "first_up",
    "first_down",
    "mix_gain",
    "w_input",
    "w_outgate",
    "w_write",
    "w_read",
    "w_step",
    "conv_taps",
    "conv_history",
    "step_bias",
    "rate_log",
    "mixer_state",
    "group_gain",
    "w_output",
    "second_gain",
    "second_gate",
    "second_up",
    "second_down",
)


def fused_body(kv, tp, *args):
    a = dict(zip(NAMES, args))
    n = kv * tp
    rows, chan = a["tokens"].shape
    state_shape = a["mixer_state"].shape
    heads = state_shape[1]
    hist_shape = a["conv_history"].shape
    for name in ("first_gain", "mix_gain", "second_gain", "step_bias", "rate_log"):
        a[name] = a[name].reshape(1, -1)
    for name in ("first_gate", "first_up", "w_step", "second_gate", "second_up"):
        a[name] = a[name].T
    a["group_gain"] = a["group_gain"].reshape(-1, LANES)
    a["mixer_state"] = a["mixer_state"].reshape(-1, state_shape[3])
    rows_in = a["w_input"].shape[1] // LANES
    rows_conv = hist_shape[2] // LANES
    pack = -(-(rows_conv + rows_in + 1) // 16) * 16

    def held(name):
        return pltpu.VMEM(a[name].shape, a[name].dtype)

    in_hbm = pl.BlockSpec(memory_space=pltpu.HBM)
    in_vmem = pl.BlockSpec(memory_space=pltpu.VMEM)
    shapes = (
        ((rows, chan), BF16),
        (a["mixer_state"].shape, F32),
        (hist_shape[1:], BF16),
    )
    kept_bytes = sum(math.prod(shape) * jnp.dtype(kind).itemsize for shape, kind in shapes)
    kept_bytes += 64 * 1024
    out = pl.pallas_call(
        functools.partial(layer_kernel, kv, tp, heads),
        out_shape=tuple(pltpu.VMEM(*shape) for shape in shapes),
        in_specs=[in_hbm] * len(NAMES),
        out_specs=(in_vmem,) * 3,
        scratch_shapes=[
            held("first_gain"),
            held("first_gate"),
            held("first_up"),
            held("first_down"),
            held("mix_gain"),
            held("w_input"),
            held("w_outgate"),
            held("w_write"),
            held("w_read"),
            held("w_step"),
            held("conv_taps"),
            pltpu.VMEM(hist_shape[1:], BF16),
            held("step_bias"),
            held("rate_log"),
            held("mixer_state"),
            held("group_gain"),
            held("w_output"),
            held("second_gain"),
            held("second_gate"),
            held("second_up"),
            held("second_down"),
            pltpu.VMEM((n, rows, chan), BF16),
            pltpu.VMEM((n - 1, rows, chan), BF16),
            pltpu.VMEM((n, rows, chan), BF16),
            pltpu.VMEM((n - 1, pack, LANES), BF16),
            pltpu.VMEM((n, pack, LANES), BF16),
            pltpu.VMEM((n, rows_in, LANES), BF16),
            pltpu.VMEM((n, rows, chan), BF16),
            pltpu.VMEM((n - 1, rows, chan), BF16),
            pltpu.VMEM((n, rows, chan), BF16),
            pltpu.VMEM((rows, pack, LANES), F32),
            pltpu.VMEM((rows, LANES), F32),
            pltpu.VMEM(a["mixer_state"].shape, BF16),
            pltpu.VMEM((hist_shape[1], rows_conv, LANES), F32),
            pltpu.VMEM((hist_shape[1] + 1, rows_conv, LANES), F32),
            pltpu.VMEM((rows_conv, LANES), F32),
            pltpu.VMEM((rows, LANES), F32),
            pltpu.VMEM(hist_shape[1:], F32),
            pltpu.VMEM((n, rows_in, LANES), F32),
            pltpu.SemaphoreType.DMA((len(NAMES),)),
            pltpu.SemaphoreType.DMA((6, n - 1)),
            pltpu.SemaphoreType.DMA((6, n)),
        ],
        compiler_params=pltpu.CompilerParams(
            collective_id=0, has_side_effects=True, vmem_limit_bytes=VMEM_BYTES - kept_bytes
        ),
        name="layer",
    )(*(a[name] for name in NAMES))
    layer_out, state_out, history_out = pl.pallas_call(
        write_kernel,
        out_shape=(
            jax.ShapeDtypeStruct((rows, chan), BF16),
            jax.ShapeDtypeStruct(a["mixer_state"].shape, F32),
            jax.ShapeDtypeStruct(hist_shape, BF16),
        ),
        in_specs=[in_vmem] * 3,
        out_specs=(in_hbm,) * 3,
        scratch_shapes=[pltpu.SemaphoreType.DMA((3,))],
        compiler_params=pltpu.CompilerParams(vmem_limit_bytes=4 * 1024 * 1024),
        name="write",
    )(*out)
    return layer_out, state_out.reshape(state_shape), history_out


def half_block_parts(resid, gain, w_gate, w_up, w_down):
    whole = lax.all_gather(resid, ("kv", "tp"), axis=1, tiled=True)
    whole_f = whole.astype(jnp.float32)
    scale = lax.rsqrt(jnp.mean(whole_f * whole_f, axis=-1, keepdims=True) + EPS)
    normed = (whole_f * scale * gain).astype(jnp.bfloat16)
    gate = jnp.dot(normed, w_gate, preferred_element_type=jnp.float32)
    upper = jnp.dot(normed, w_up, preferred_element_type=jnp.float32)
    hidden = (jax.nn.silu(gate) * upper).astype(jnp.bfloat16)
    down = jnp.dot(hidden, w_down, preferred_element_type=jnp.float32)
    share = lax.psum_scatter(down, ("kv", "tp"), scatter_dimension=1, tiled=True)
    return (resid.astype(jnp.float32) + 0.5 * share).astype(jnp.bfloat16)


def body(
    tokens,
    first_gain,
    first_gate,
    first_up,
    first_down,
    mix_gain,
    w_input,
    w_outgate,
    w_write,
    w_read,
    w_step,
    conv_taps,
    conv_history,
    step_bias,
    rate_log,
    mixer_state,
    group_gain,
    w_output,
    second_gain,
    second_gate,
    second_up,
    second_down,
):
    width = first_gate.shape[0]
    count = mixer_state.shape[0]
    heads = mixer_state.shape[1]
    head_dim = mixer_state.shape[2]
    state_dim = mixer_state.shape[3]
    ssd_width = heads * head_dim
    groups = w_write.shape[1] // state_dim
    per_group = heads // groups
    first = half_block_parts(tokens, first_gain, first_gate, first_up, first_down)
    first_f = first.astype(jnp.float32)
    squares = jnp.sum(first_f * first_f, axis=1)
    premix = (first_f * mix_gain).astype(jnp.bfloat16)
    part_input = jnp.dot(premix, w_input, preferred_element_type=jnp.float32)
    part_write = jnp.dot(premix, w_write, preferred_element_type=jnp.float32)
    part_read = jnp.dot(premix, w_read, preferred_element_type=jnp.float32)
    part_step = jnp.dot(premix, w_step, preferred_element_type=jnp.float32)
    part_gate = jnp.dot(premix, w_outgate, preferred_element_type=jnp.float32)
    totals = lax.psum(squares, ("kv", "tp"))
    head_terms = (part_input, part_write, part_read, part_step)
    extra_terms = ()
    summed = lax.psum_scatter(
        head_terms + extra_terms + (part_gate,), ("kv", "tp"), scatter_dimension=0, tiled=True
    )
    gate_sum = summed[-1]
    summed = summed[:-1]
    own_squares = lax.dynamic_slice_in_dim(totals, lax.axis_index(("kv", "tp")) * count, count, 0)
    scale = lax.rsqrt(own_squares / width + EPS)[:, None]
    inputs = (scale * summed[0]).astype(jnp.bfloat16)
    writes = (scale * summed[1]).astype(jnp.bfloat16)
    reads = (scale * summed[2]).astype(jnp.bfloat16)
    steps_raw = (scale * summed[3]).astype(jnp.bfloat16)
    fresh = jnp.concatenate([inputs, writes, reads], axis=1)
    window = jnp.concatenate([conv_history, fresh[:, None, :]], axis=1)
    history_out = window[:, 1:]
    conv = jax.nn.silu(
        jnp.sum(window.astype(jnp.float32) * conv_taps.astype(jnp.float32)[None], axis=1)
    )
    conv_in = conv[:, :ssd_width].reshape(count, groups, per_group, head_dim)
    conv_write = conv[:, ssd_width : ssd_width + groups * state_dim].reshape(
        count, groups, state_dim
    )
    conv_read = conv[:, ssd_width + groups * state_dim :].reshape(count, groups, state_dim)
    step = jax.nn.softplus(steps_raw.astype(jnp.float32) + step_bias)
    decay = jnp.exp(-step * jnp.exp(rate_log))
    state = mixer_state.reshape(count, groups, per_group, head_dim, state_dim)
    decay_g = decay.reshape(count, groups, per_group)
    step_g = step.reshape(count, groups, per_group)
    written = (step_g[..., None] * conv_in)[..., None] * conv_write[:, :, None, None, :]
    new_state = decay_g[..., None, None] * state + written
    read_out = jnp.einsum("sgjpn,sgn->sgjp", new_state, conv_read, precision=lax.Precision.HIGHEST)
    outgate = (scale * gate_sum).astype(jnp.bfloat16)
    gated = read_out.reshape(count, ssd_width) * jax.nn.silu(outgate.astype(jnp.float32))
    blocks = gated.reshape(count, groups, ssd_width // groups)
    block_scale = lax.rsqrt(jnp.mean(blocks * blocks, axis=-1, keepdims=True) + EPS)
    normed = ((blocks * block_scale).reshape(count, ssd_width) * group_gain).astype(jnp.bfloat16)
    mixed = jnp.dot(
        lax.all_gather(normed, ("kv", "tp"), axis=0, tiled=True),
        w_output,
        preferred_element_type=jnp.float32,
    )
    second = (first_f + mixed).astype(jnp.bfloat16)
    layer_out = half_block_parts(second, second_gain, second_gate, second_up, second_down)
    state_out = new_state.reshape(count, heads, head_dim, state_dim)
    return (layer_out, state_out, history_out)


def run_body(kv, tp, *args):
    tokens, state, taps = args[0], args[15], args[11]
    w_input, w_write = args[6], args[8]
    rows, chan = tokens.shape
    count, heads, head_dim, state_dim = state.shape
    fits = (
        count == 1
        and rows == kv * tp
        and rows == 8
        and chan % LANES == 0
        and state_dim == LANES
        and LANES % head_dim == 0
        and taps.shape[0] == 4
        and heads + 2 <= LANES
        and (w_input.shape[1] // LANES) % (w_write.shape[1] // LANES) == 0
    )
    if fits:
        return fused_body(kv, tp, *args)
    return body(*args)


def solution(mesh):
    return jax.shard_map(
        functools.partial(run_body, mesh.shape["kv"], mesh.shape["tp"]),
        mesh=mesh,
        in_specs=(
            P("dp", ("kv", "tp")),
            P(),
            P(None, ("kv", "tp")),
            P(None, ("kv", "tp")),
            P(("kv", "tp"), None),
            P(("kv", "tp")),
            P(("kv", "tp"), None),
            P(("kv", "tp"), None),
            P(("kv", "tp"), None),
            P(("kv", "tp"), None),
            P(("kv", "tp"), None),
            P(),
            P(("dp", "kv", "tp"), None, None),
            P(),
            P(),
            P(("dp", "kv", "tp"), None, None, None),
            P(),
            P(None, ("kv", "tp")),
            P(),
            P(None, ("kv", "tp")),
            P(None, ("kv", "tp")),
            P(("kv", "tp"), None),
        ),
        out_specs=(
            P("dp", ("kv", "tp")),
            P(("dp", "kv", "tp"), None, None, None),
            P(("dp", "kv", "tp"), None, None),
        ),
        check_vma=False,
    )
```

```python
import functools
import math

import jax
import jax.numpy as jnp
from jax import lax
from jax.experimental import pallas as pl
from jax.experimental.pallas import tpu as pltpu
from jax.sharding import PartitionSpec as P

EPS = 1e-06
F32 = jnp.float32
BF16 = jnp.bfloat16
LANES = 128
VMEM_BYTES = 67043328
MESH = pl.DeviceIdType.MESH


def silu(x):
    return x * jax.nn.sigmoid(x)


def dot_rows(left, right):
    contract = (((1,), (1,)), ((), ()))
    return lax.dot_general(left, right, contract, preferred_element_type=F32)


def layer_kernel(
    kv,
    tp,
    heads,
    tokens,
    first_gain,
    first_gate,
    first_up,
    first_down,
    mix_gain,
    w_input,
    w_outgate,
    w_write,
    w_read,
    w_step,
    conv_taps,
    conv_history,
    step_bias,
    rate_log,
    mixer_state,
    group_gain,
    w_output,
    second_gain,
    second_gate,
    second_up,
    second_down,
    layer_out,
    state_out,
    history_out,
    g1,
    wg1,
    wu1,
    wd1,
    mg,
    wi,
    wo,
    ww,
    wr,
    ws,
    taps,
    hist,
    bias,
    rate,
    state,
    ggain,
    wout,
    g2,
    wg2,
    wu2,
    wd2,
    tok_all,
    down_send1,
    down_recv1,
    proj_send,
    proj_recv,
    norm_all,
    sec_all,
    down_send2,
    down_recv2,
    proj_f,
    step_f,
    state_b,
    hist_f,
    taps_f,
    fresh_f,
    dots_f,
    tail_f,
    norm_f,
    load_sem,
    send_sem,
    recv_sem,
):
    n = kv * tp
    rows, chan = tokens.shape
    width = n * chan
    rows_in = w_input.shape[1] // LANES
    rows_map = w_write.shape[1] // LANES
    rows_conv = rows_in + 2 * rows_map
    rows_all = rows_conv + rows_in
    pack = proj_send.shape[1]
    per_row = heads // rows_in
    head_dim = LANES // per_row
    group_rows = rows_in // rows_map

    my_kv = lax.axis_index("kv")
    my_tp = lax.axis_index("tp")
    me = my_kv * tp + my_tp

    if kv == 4:
        half = my_kv // 2
        chips = [my_kv + 1 - 2 * lax.rem(my_kv, 2), 2 - half, 3 - 3 * half]
    else:
        chips = [lax.rem(my_kv + d, kv) for d in range(1, kv)]
    peers = []
    for pk in reversed(chips):
        for t in range(tp):
            peers.append((pk * tp + t, {"kv": pk, "tp": t}))
    for t in range(1, tp):
        pt = lax.rem(my_tp + t, tp)
        peers.append((my_kv * tp + pt, {"kv": my_kv, "tp": pt}))

    loads = {}

    def load(name, src, dst):
        copy = pltpu.make_async_copy(src, dst, load_sem.at[len(loads)])
        copy.start()
        loads[name] = copy

    def ready(*names):
        for name in names:
            loads[name].wait()

    sends = []

    def send(phase, index, src, dst):
        peer, where = peers[index]
        copy = pltpu.make_async_remote_copy(
            src_ref=src,
            dst_ref=dst,
            send_sem=send_sem.at[phase, index],
            recv_sem=recv_sem.at[phase, me],
            device_id=where,
            device_id_type=MESH,
        )
        copy.start()
        sends.append(copy)

    def arrive(phase, index, dst):
        peer, where = peers[index]
        pltpu.make_async_remote_copy(
            src_ref=dst,
            dst_ref=dst,
            send_sem=send_sem.at[phase, index],
            recv_sem=recv_sem.at[phase, peer],
            device_id=where,
            device_id_type=MESH,
        ).wait_recv()

    barrier = pltpu.get_barrier_semaphore()
    for _, where in peers:
        pl.semaphore_signal(barrier, inc=1, device_id=where, device_id_type=MESH)
    load("tokens", tokens, tok_all.at[me])
    load("g1", first_gain, g1)
    load("hist", conv_history.at[0], hist)
    load("taps", conv_taps, taps)
    load("wg1", first_gate, wg1)
    load("wu1", first_up, wu1)
    load("wd1", first_down, wd1)
    load("mg", mix_gain, mg)
    load("bias", step_bias, bias)
    load("rate", rate_log, rate)
    load("ggain", group_gain, ggain)
    load("g2", second_gain, g2)
    ready("tokens")
    pl.semaphore_wait(barrier, n - 1)
    for i in range(n - 1):
        send(0, i, tok_all.at[me], tok_all.at[me])
    load("wi", w_input, wi)
    load("ww", w_write, ww)
    load("wr", w_read, wr)
    load("wo", w_outgate, wo)
    load("ws", w_step, ws)
    load("state", mixer_state, state)

    ready("hist", "taps")
    for k in range(rows_conv):
        lanes = slice(k * LANES, (k + 1) * LANES)
        hist_f[:, k, :] = hist[:, lanes].astype(F32)
        taps_f[:, k, :] = taps[:, lanes].astype(F32)

    def half_block(phase, slots, gain, w_gate, w_up, w_down, names, down_send, down_recv, fill):
        ready(*names[:3])
        block = tp * chan
        power = gate = upper = None
        steps = [[(None, me)]] + [[(i, peers[i][0])] for i in reversed(range(n - 1))]
        for step in steps:
            for i, owner in step:
                if i is not None:
                    arrive(phase, i, slots.at[owner])
            resid = jnp.concatenate([slots[owner] for _, owner in step], axis=1).astype(F32)
            start = pl.multiple_of(step[0][1] * chan, chan)
            columns = pl.ds(start, len(step) * chan)
            weighted = (resid * gain[:, columns]).astype(BF16)
            terms = (
                jnp.sum(resid * resid, axis=1, keepdims=True),
                dot_rows(weighted, w_gate[:, columns]),
                dot_rows(weighted, w_up[:, columns]),
            )
            if power is None:
                power, gate, upper = terms
            else:
                power, gate, upper = power + terms[0], gate + terms[1], upper + terms[2]
        scale = lax.rsqrt(power / width + EPS)
        hidden = (silu(gate * scale) * (upper * scale)).astype(BF16)
        ready(names[3])

        def part(dest):
            columns = pl.ds(pl.multiple_of(dest * chan, chan), chan)
            return jnp.dot(hidden, w_down[:, columns], preferred_element_type=F32)

        for c, pk in enumerate(reversed(chips)):
            columns = pl.ds(pl.multiple_of(pk * block, block), block)
            wide = jnp.dot(hidden, w_down[:, columns], preferred_element_type=F32).astype(BF16)
            for t in range(tp):
                i = c * tp + t
                down_send[i] = wide[:, t * chan : (t + 1) * chan]
                send(phase + 1, i, down_send.at[i], down_recv.at[me])
        for i in range(len(chips) * tp, n - 1):
            down_send[i] = part(peers[i][0]).astype(BF16)
            send(phase + 1, i, down_send.at[i], down_recv.at[me])
        total = part(me)
        fill()
        for i in reversed(range(n - 1)):
            peer = peers[i][0]
            arrive(phase + 1, i, down_recv.at[peer])
            total = total + down_recv[peer].astype(F32)
        own = slots[me].astype(F32)
        return (own + 0.5 * total).astype(BF16)

    load("wout", w_output, wout)
    load("wg2", second_gate, wg2)
    load("wu2", second_up, wu2)
    load("wd2", second_down, wd2)

    def round_state():
        ready("state")
        for r in range(rows_in):
            block = slice(r * LANES, (r + 1) * LANES)
            state_b[:, block] = jnp.transpose(state[block]).astype(BF16)

    first = half_block(
        0,
        tok_all,
        g1,
        wg1,
        wu1,
        wd1,
        ("g1", "wg1", "wu1", "wd1"),
        down_send1,
        down_recv1,
        round_state,
    )
    first_f = first.astype(F32)

    ready("mg", "wi", "ww", "wr", "wo", "ws")
    squares = jnp.sum(first_f * first_f, axis=1, keepdims=True)
    premix = (first_f * mg[...]).astype(BF16)
    row = 0
    for weight in (wi, ww, wr, wo):
        part = jnp.dot(premix, weight[...], preferred_element_type=F32)
        for k in range(weight.shape[1] // LANES):
            proj_f[:, row, :] = part[:, k * LANES : (k + 1) * LANES]
            row += 1
    step_f[...] = jnp.zeros_like(step_f)
    step_f[:, :heads] = dot_rows(premix, ws[...])
    high = squares.astype(BF16).astype(F32)
    lane = lax.broadcasted_iota(jnp.int32, (rows, LANES), 1)
    last = jnp.where(lane == heads, high, step_f[...])
    last = jnp.where(lane == heads + 1, squares - high, last)
    proj_f[:, row, :] = last
    for k in range(row + 1, pack):
        proj_f[:, k, :] = jnp.zeros((rows, LANES), F32)
    for i, (peer, _) in enumerate(peers):
        proj_send[i] = proj_f[peer].astype(BF16)
        send(2, i, proj_send.at[i], proj_recv.at[me])
    summed = proj_f[me]
    for i in reversed(range(n - 1)):
        peer = peers[i][0]
        arrive(2, i, proj_recv.at[peer])
        summed = summed + proj_recv[peer].astype(F32)

    tail = summed[rows_all : rows_all + 1]
    own_squares = tail[:, heads : heads + 1] + tail[:, heads + 1 : heads + 2]
    scale = lax.rsqrt(own_squares / width + EPS)
    scaled = (scale * summed).astype(BF16).astype(F32)
    fresh = scaled[:rows_conv]
    conv = taps_f[3] * fresh
    for k in range(3):
        conv = conv + taps_f[k] * hist_f[k]
    conv = silu(conv)
    conv_in = conv[:rows_in]
    conv_write = conv[rows_in : rows_in + rows_map]
    conv_read = conv[rows_in + rows_map :]
    outgate = scaled[rows_conv:rows_all]

    ready("bias", "rate", "ggain")
    steps_raw = scaled[rows_all : rows_all + 1, :heads] + bias[...]
    step_row = jnp.maximum(steps_raw, 0.0) + jnp.log1p(jnp.exp(-jnp.abs(steps_raw)))
    decay_row = jnp.exp(-step_row * jnp.exp(rate[...]))
    r_id = lax.broadcasted_iota(jnp.int32, (rows_in, heads), 0)
    h_id = lax.broadcasted_iota(jnp.int32, (rows_in, heads), 1)
    wide_lane = lax.broadcasted_iota(jnp.int32, (rows_in, LANES), 1)

    def spread(values):
        out = jnp.zeros((rows_in, LANES), F32)
        for k in range(per_row):
            mine = jnp.where(h_id == r_id * per_row + k, values, 0.0)
            column = jnp.sum(mine, axis=1, keepdims=True)
            inside = (wide_lane >= k * head_dim) & (wide_lane < (k + 1) * head_dim)
            out = jnp.where(inside, column, out)
        return out

    step_c = spread(step_row)
    decay_c = spread(decay_row)
    fed = step_c * conv_in

    read_high = conv_read.astype(BF16).astype(F32)
    lhs = jnp.concatenate([read_high, conv_read - read_high], axis=0).astype(BF16)
    dots = jnp.dot(lhs, state_b[...], preferred_element_type=F32)
    pieces = []
    for r in range(rows_in):
        g = r // group_rows
        lanes = slice(r * LANES, (r + 1) * LANES)
        pieces.append(dots[g : g + 1, lanes] + dots[rows_map + g : rows_map + g + 1, lanes])
    old_read = jnp.concatenate(pieces, axis=0)
    both = jnp.sum(conv_write * conv_read, axis=1, keepdims=True)
    both = jnp.concatenate(
        [jnp.broadcast_to(both[g : g + 1], (group_rows, 1)) for g in range(rows_map)], axis=0
    )
    read_out = decay_c * old_read + fed * both
    gated = read_out * silu(outgate)
    power = jnp.sum(gated * gated, axis=1, keepdims=True)
    power = jnp.concatenate(
        [
            jnp.broadcast_to(
                jnp.sum(power[g * group_rows : (g + 1) * group_rows], axis=0, keepdims=True),
                (group_rows, 1),
            )
            for g in range(rows_map)
        ],
        axis=0,
    )
    block_scale = lax.rsqrt(power / (group_rows * LANES) + EPS)
    norm_all[me] = (gated * block_scale * ggain[...]).astype(BF16)
    for i in range(n - 1):
        send(3, i, norm_all.at[me], norm_all.at[me])

    decay_t = jnp.transpose(decay_c)
    fed_t = jnp.transpose(fed)
    for r in range(rows_in):
        g = r // group_rows
        block = slice(r * LANES, (r + 1) * LANES)
        state_out[block] = (
            decay_t[:, r : r + 1] * state[block]
            + fed_t[:, r : r + 1] * conv_write[g : g + 1]
        )
    fresh_f[...] = fresh
    kept = hist.shape[0]
    tail_f[0 : kept - 1, :] = hist[...].astype(F32)[1:]
    for k in range(rows_conv):
        tail_f[kept - 1 : kept, k * LANES : (k + 1) * LANES] = fresh_f[k : k + 1, :]
    history_out[...] = tail_f[...].astype(BF16)

    for i in reversed(range(n - 1)):
        arrive(3, i, norm_all.at[peers[i][0]])
    for j in range(n):
        norm_f[j] = norm_all[j].astype(F32)
    normed = jnp.concatenate([norm_f[:, r, :] for r in range(rows_in)], axis=1).astype(BF16)
    ready("wout")
    mixed = jnp.dot(normed, wout[...], preferred_element_type=F32)
    sec_all[me] = (first_f + mixed).astype(BF16)
    for i in range(n - 1):
        send(4, i, sec_all.at[me], sec_all.at[me])
    layer_out[...] = half_block(
        4,
        sec_all,
        g2,
        wg2,
        wu2,
        wd2,
        ("g2", "wg2", "wu2", "wd2"),
        down_send2,
        down_recv2,
        lambda: None,
    )
    for copy in sends:
        copy.wait_send()


def write_kernel(layer_in, state_in, history_in, layer_out, state_out, history_out, sem):
    copies = [
        pltpu.make_async_copy(state_in, state_out, sem.at[0]),
        pltpu.make_async_copy(layer_in, layer_out, sem.at[1]),
        pltpu.make_async_copy(history_in, history_out.at[0], sem.at[2]),
    ]
    for copy in copies:
        copy.start()
    for copy in copies:
        copy.wait()


NAMES = (
    "tokens",
    "first_gain",
    "first_gate",
    "first_up",
    "first_down",
    "mix_gain",
    "w_input",
    "w_outgate",
    "w_write",
    "w_read",
    "w_step",
    "conv_taps",
    "conv_history",
    "step_bias",
    "rate_log",
    "mixer_state",
    "group_gain",
    "w_output",
    "second_gain",
    "second_gate",
    "second_up",
    "second_down",
)


def fused_body(kv, tp, *args):
    a = dict(zip(NAMES, args))
    n = kv * tp
    rows, chan = a["tokens"].shape
    state_shape = a["mixer_state"].shape
    heads = state_shape[1]
    hist_shape = a["conv_history"].shape
    for name in ("first_gain", "mix_gain", "second_gain", "step_bias", "rate_log"):
        a[name] = a[name].reshape(1, -1)
    for name in ("first_gate", "first_up", "w_step", "second_gate", "second_up"):
        a[name] = a[name].T
    a["group_gain"] = a["group_gain"].reshape(-1, LANES)
    a["mixer_state"] = a["mixer_state"].reshape(-1, state_shape[3])
    rows_in = a["w_input"].shape[1] // LANES
    rows_conv = hist_shape[2] // LANES
    pack = -(-(rows_conv + rows_in + 1) // 16) * 16

    def held(name):
        return pltpu.VMEM(a[name].shape, a[name].dtype)

    in_hbm = pl.BlockSpec(memory_space=pltpu.HBM)
    in_vmem = pl.BlockSpec(memory_space=pltpu.VMEM)
    shapes = (
        ((rows, chan), BF16),
        (a["mixer_state"].shape, F32),
        (hist_shape[1:], BF16),
    )
    kept_bytes = sum(math.prod(shape) * jnp.dtype(kind).itemsize for shape, kind in shapes)
    kept_bytes += 64 * 1024
    out = pl.pallas_call(
        functools.partial(layer_kernel, kv, tp, heads),
        out_shape=tuple(pltpu.VMEM(*shape) for shape in shapes),
        in_specs=[in_hbm] * len(NAMES),
        out_specs=(in_vmem,) * 3,
        scratch_shapes=[
            held("first_gain"),
            held("first_gate"),
            held("first_up"),
            held("first_down"),
            held("mix_gain"),
            held("w_input"),
            held("w_outgate"),
            held("w_write"),
            held("w_read"),
            held("w_step"),
            held("conv_taps"),
            pltpu.VMEM(hist_shape[1:], BF16),
            held("step_bias"),
            held("rate_log"),
            held("mixer_state"),
            held("group_gain"),
            held("w_output"),
            held("second_gain"),
            held("second_gate"),
            held("second_up"),
            held("second_down"),
            pltpu.VMEM((n, rows, chan), BF16),
            pltpu.VMEM((n - 1, rows, chan), BF16),
            pltpu.VMEM((n, rows, chan), BF16),
            pltpu.VMEM((n - 1, pack, LANES), BF16),
            pltpu.VMEM((n, pack, LANES), BF16),
            pltpu.VMEM((n, rows_in, LANES), BF16),
            pltpu.VMEM((n, rows, chan), BF16),
            pltpu.VMEM((n - 1, rows, chan), BF16),
            pltpu.VMEM((n, rows, chan), BF16),
            pltpu.VMEM((rows, pack, LANES), F32),
            pltpu.VMEM((rows, LANES), F32),
            pltpu.VMEM(a["mixer_state"].shape[::-1], BF16),
            pltpu.VMEM((hist_shape[1], rows_conv, LANES), F32),
            pltpu.VMEM((hist_shape[1] + 1, rows_conv, LANES), F32),
            pltpu.VMEM((rows_conv, LANES), F32),
            pltpu.VMEM((rows, LANES), F32),
            pltpu.VMEM(hist_shape[1:], F32),
            pltpu.VMEM((n, rows_in, LANES), F32),
            pltpu.SemaphoreType.DMA((len(NAMES),)),
            pltpu.SemaphoreType.DMA((6, n - 1)),
            pltpu.SemaphoreType.DMA((6, n)),
        ],
        compiler_params=pltpu.CompilerParams(
            collective_id=0, has_side_effects=True, vmem_limit_bytes=VMEM_BYTES - kept_bytes
        ),
        name="layer",
    )(*(a[name] for name in NAMES))
    layer_out, state_out, history_out = pl.pallas_call(
        write_kernel,
        out_shape=(
            jax.ShapeDtypeStruct((rows, chan), BF16),
            jax.ShapeDtypeStruct(a["mixer_state"].shape, F32),
            jax.ShapeDtypeStruct(hist_shape, BF16),
        ),
        in_specs=[in_vmem] * 3,
        out_specs=(in_hbm,) * 3,
        scratch_shapes=[pltpu.SemaphoreType.DMA((3,))],
        compiler_params=pltpu.CompilerParams(vmem_limit_bytes=4 * 1024 * 1024),
        name="write",
    )(*out)
    return layer_out, state_out.reshape(state_shape), history_out


def half_block_parts(resid, gain, w_gate, w_up, w_down):
    whole = lax.all_gather(resid, ("kv", "tp"), axis=1, tiled=True)
    whole_f = whole.astype(jnp.float32)
    scale = lax.rsqrt(jnp.mean(whole_f * whole_f, axis=-1, keepdims=True) + EPS)
    normed = (whole_f * scale * gain).astype(jnp.bfloat16)
    gate = jnp.dot(normed, w_gate, preferred_element_type=jnp.float32)
    upper = jnp.dot(normed, w_up, preferred_element_type=jnp.float32)
    hidden = (jax.nn.silu(gate) * upper).astype(jnp.bfloat16)
    down = jnp.dot(hidden, w_down, preferred_element_type=jnp.float32)
    share = lax.psum_scatter(down, ("kv", "tp"), scatter_dimension=1, tiled=True)
    return (resid.astype(jnp.float32) + 0.5 * share).astype(jnp.bfloat16)


def body(
    tokens,
    first_gain,
    first_gate,
    first_up,
    first_down,
    mix_gain,
    w_input,
    w_outgate,
    w_write,
    w_read,
    w_step,
    conv_taps,
    conv_history,
    step_bias,
    rate_log,
    mixer_state,
    group_gain,
    w_output,
    second_gain,
    second_gate,
    second_up,
    second_down,
):
    width = first_gate.shape[0]
    count = mixer_state.shape[0]
    heads = mixer_state.shape[1]
    head_dim = mixer_state.shape[2]
    state_dim = mixer_state.shape[3]
    ssd_width = heads * head_dim
    groups = w_write.shape[1] // state_dim
    per_group = heads // groups
    first = half_block_parts(tokens, first_gain, first_gate, first_up, first_down)
    first_f = first.astype(jnp.float32)
    squares = jnp.sum(first_f * first_f, axis=1)
    premix = (first_f * mix_gain).astype(jnp.bfloat16)
    part_input = jnp.dot(premix, w_input, preferred_element_type=jnp.float32)
    part_write = jnp.dot(premix, w_write, preferred_element_type=jnp.float32)
    part_read = jnp.dot(premix, w_read, preferred_element_type=jnp.float32)
    part_step = jnp.dot(premix, w_step, preferred_element_type=jnp.float32)
    part_gate = jnp.dot(premix, w_outgate, preferred_element_type=jnp.float32)
    totals = lax.psum(squares, ("kv", "tp"))
    head_terms = (part_input, part_write, part_read, part_step)
    extra_terms = ()
    summed = lax.psum_scatter(
        head_terms + extra_terms + (part_gate,), ("kv", "tp"), scatter_dimension=0, tiled=True
    )
    gate_sum = summed[-1]
    summed = summed[:-1]
    own_squares = lax.dynamic_slice_in_dim(totals, lax.axis_index(("kv", "tp")) * count, count, 0)
    scale = lax.rsqrt(own_squares / width + EPS)[:, None]
    inputs = (scale * summed[0]).astype(jnp.bfloat16)
    writes = (scale * summed[1]).astype(jnp.bfloat16)
    reads = (scale * summed[2]).astype(jnp.bfloat16)
    steps_raw = (scale * summed[3]).astype(jnp.bfloat16)
    fresh = jnp.concatenate([inputs, writes, reads], axis=1)
    window = jnp.concatenate([conv_history, fresh[:, None, :]], axis=1)
    history_out = window[:, 1:]
    conv = jax.nn.silu(
        jnp.sum(window.astype(jnp.float32) * conv_taps.astype(jnp.float32)[None], axis=1)
    )
    conv_in = conv[:, :ssd_width].reshape(count, groups, per_group, head_dim)
    conv_write = conv[:, ssd_width : ssd_width + groups * state_dim].reshape(
        count, groups, state_dim
    )
    conv_read = conv[:, ssd_width + groups * state_dim :].reshape(count, groups, state_dim)
    step = jax.nn.softplus(steps_raw.astype(jnp.float32) + step_bias)
    decay = jnp.exp(-step * jnp.exp(rate_log))
    state = mixer_state.reshape(count, groups, per_group, head_dim, state_dim)
    decay_g = decay.reshape(count, groups, per_group)
    step_g = step.reshape(count, groups, per_group)
    written = (step_g[..., None] * conv_in)[..., None] * conv_write[:, :, None, None, :]
    new_state = decay_g[..., None, None] * state + written
    read_out = jnp.einsum("sgjpn,sgn->sgjp", new_state, conv_read, precision=lax.Precision.HIGHEST)
    outgate = (scale * gate_sum).astype(jnp.bfloat16)
    gated = read_out.reshape(count, ssd_width) * jax.nn.silu(outgate.astype(jnp.float32))
    blocks = gated.reshape(count, groups, ssd_width // groups)
    block_scale = lax.rsqrt(jnp.mean(blocks * blocks, axis=-1, keepdims=True) + EPS)
    normed = ((blocks * block_scale).reshape(count, ssd_width) * group_gain).astype(jnp.bfloat16)
    mixed = jnp.dot(
        lax.all_gather(normed, ("kv", "tp"), axis=0, tiled=True),
        w_output,
        preferred_element_type=jnp.float32,
    )
    second = (first_f + mixed).astype(jnp.bfloat16)
    layer_out = half_block_parts(second, second_gain, second_gate, second_up, second_down)
    state_out = new_state.reshape(count, heads, head_dim, state_dim)
    return (layer_out, state_out, history_out)


def run_body(kv, tp, *args):
    tokens, state, taps = args[0], args[15], args[11]
    w_input, w_write = args[6], args[8]
    rows, chan = tokens.shape
    count, heads, head_dim, state_dim = state.shape
    fits = (
        count == 1
        and rows == kv * tp
        and rows == 8
        and chan % LANES == 0
        and state_dim == LANES
        and LANES % head_dim == 0
        and taps.shape[0] == 4
        and heads + 2 <= LANES
        and (w_input.shape[1] // LANES) % (w_write.shape[1] // LANES) == 0
    )
    if fits:
        return fused_body(kv, tp, *args)
    return body(*args)


def solution(mesh):
    return jax.shard_map(
        functools.partial(run_body, mesh.shape["kv"], mesh.shape["tp"]),
        mesh=mesh,
        in_specs=(
            P("dp", ("kv", "tp")),
            P(),
            P(None, ("kv", "tp")),
            P(None, ("kv", "tp")),
            P(("kv", "tp"), None),
            P(("kv", "tp")),
            P(("kv", "tp"), None),
            P(("kv", "tp"), None),
            P(("kv", "tp"), None),
            P(("kv", "tp"), None),
            P(("kv", "tp"), None),
            P(),
            P(("dp", "kv", "tp"), None, None),
            P(),
            P(),
            P(("dp", "kv", "tp"), None, None, None),
            P(),
            P(None, ("kv", "tp")),
            P(),
            P(None, ("kv", "tp")),
            P(None, ("kv", "tp")),
            P(("kv", "tp"), None),
        ),
        out_specs=(
            P("dp", ("kv", "tp")),
            P(("dp", "kv", "tp"), None, None, None),
            P(("dp", "kv", "tp"), None, None),
        ),
        check_vma=False,
    )
```
